32 devices in a mesh: sp: 8 (over z, x), tp: 4 (over y, core).
Axes of the slice: x: 2, y: 2, z: 4, core: 2. Of those that a mesh axis runs over, the one named last changes fastest.
Arguments:
- inputs: bfloat16 [4096, 2048], P('sp', 'tp'), may hold values from -45 to 45
- norm_gain: float32 [3, 2048], replicated, may hold values from 0.1 to 1.9
- w_value: bfloat16 [3, 2048, 1024], P(None, 'sp', 'tp'), may hold values from -0.125 to 0.125
- w_gate: bfloat16 [3, 2048, 1024], P(None, 'sp', 'tp'), may hold values from -0.125 to 0.125
- conv_taps: float32 [3, 31, 1024], P(None, None, 'tp'), may hold values from -5 to 5
- ln_gain: float32 [3, 1024], P(None, 'tp'), may hold values from 0.1 to 1.9
- ln_bias: float32 [3, 1024], P(None, 'tp'), may hold values from -3 to 3
- w_out: bfloat16 [3, 1024, 2048], P(None, 'tp', 'sp'), may hold values from -0.1875 to 0.1875
Outputs:
- stream: bfloat16 [4096, 2048], P('sp', 'tp')
The draws below stay inside these ranges and needn't reach their ends.
All inputs are finite; a program needn't handle non-finite values.
Results may differ from the reference program's by a relative error of at most 0.01.
Values may be sent and summed in bfloat16 or wider, within the bound.
A program may use at most 64 MiB of HBM per device.

```python
import jax
import jax.numpy as jnp
from jax import lax

D = 2048
C = 1024
K = 31
LAYERS = 3
TOKENS = 4096
N_TP = 4


def draw_inputs(key, part):
    key_a, key_b = jax.random.split(jax.random.fold_in(key, 11), 2)
    ramp = 10.0 ** (0.5 * jnp.arange(D, dtype=jnp.float32) / D + 0.3 * jax.random.uniform(key_b, (D,), jnp.float32))
    base = jnp.clip(jax.random.normal(key_a, (TOKENS, D), jnp.float32), -4.0, 4.0)
    return (base * ramp[None, :]).astype(jnp.bfloat16)


def draw_conv_taps(key, part):
    key_a, key_b = jax.random.split(jax.random.fold_in(key, 23), 2)
    ramp = K ** (-0.5) * 10.0 ** (0.5 * jnp.arange(C, dtype=jnp.float32) / C + 0.3 * jax.random.uniform(key_b, (LAYERS, 1, C), jnp.float32))
    base = jnp.clip(jax.random.normal(key_a, (LAYERS, K, C), jnp.float32), -4.0, 4.0)
    return base * ramp


def levels(key, shape, cuts, low, high):
    factor_of = 1.0
    for dim, blocks in cuts:
        draws = jax.random.uniform(jax.random.fold_in(jax.random.fold_in(key, 6), dim), (blocks,), jnp.float32, low / len(cuts), high / len(cuts))
        factor_of = factor_of * jnp.repeat(jnp.exp(draws), shape[dim] // blocks).reshape((-1,) + (1,) * (len(shape) - 1 - dim))
    return factor_of


def normal_values(stream_key, shape, width, bound, cuts=(), kind=jnp.bfloat16):
    loudness = levels(stream_key, shape, cuts, -0.22, 0.18) if cuts else 1.0
    values = jax.random.normal(stream_key, shape, jnp.float32) * width * loudness
    return jnp.minimum(jnp.maximum(values, -bound), bound).astype(kind)


def setup_inputs(seed: int = 0) -> dict:
    streams_of = jax.random.split(jax.random.key(seed), 9)
    inputs = draw_inputs(jax.random.fold_in(streams_of[8], 71), 0)
    norm_gain = jnp.clip(1.0 + 0.18 * jax.random.normal(streams_of[1], (LAYERS, D), jnp.float32), 0.1, 1.9)
    w_value = normal_values(streams_of[2], (LAYERS, D, C), D ** -0.5, 0.125, ((1, 8), (2, 4)))
    w_gate = normal_values(streams_of[3], (LAYERS, D, C), D ** -0.5, 0.125, ((1, 8), (2, 4)))
    conv_taps = draw_conv_taps(jax.random.fold_in(streams_of[8], 71), 0)
    ln_gain = jnp.clip(1.0 + 0.18 * jax.random.normal(streams_of[5], (LAYERS, C), jnp.float32), 0.1, 1.9)
    ln_bias = normal_values(streams_of[6], (LAYERS, C), 0.5, 3.0, ((1, 4),), jnp.float32)
    w_out = normal_values(streams_of[7], (LAYERS, C, D), C ** -0.5, 0.1875, ((1, 4), (2, 8)))
    return {"inputs": inputs, "norm_gain": norm_gain, "w_value": w_value, "w_gate": w_gate, "conv_taps": conv_taps, "ln_gain": ln_gain, "ln_bias": ln_bias, "w_out": w_out}


def reference(inputs, norm_gain, w_value, w_gate, conv_taps, ln_gain, ln_bias, w_out):
    block = C // N_TP
    stream = inputs
    for layer in range(LAYERS):
        xf = stream.astype(jnp.float32)
        meansq = lax.optimization_barrier(jnp.mean(xf * xf, axis=1, keepdims=True))
        hidden = (xf * lax.rsqrt(meansq + 1e-06) * norm_gain[layer][None, :]).astype(jnp.bfloat16)
        value = jnp.dot(hidden, w_value[layer], preferred_element_type=jnp.float32)
        gate = jnp.dot(hidden, w_gate[layer], preferred_element_type=jnp.float32)
        glu = (value * jax.nn.sigmoid(gate)).astype(jnp.bfloat16)
        padded = jnp.pad(glu.astype(jnp.float32), ((K - 1, 0), (0, 0)))
        filtered = jnp.zeros((TOKENS, C), jnp.float32)
        for tap in range(K):
            filtered = filtered + conv_taps[layer, tap][None, :] * padded[tap:tap + TOKENS]
        mean_val = lax.optimization_barrier(jnp.mean(filtered, axis=1, keepdims=True))
        var_val = lax.optimization_barrier(jnp.mean(filtered * filtered, axis=1, keepdims=True)) - mean_val * mean_val
        normed = jax.nn.silu((filtered - mean_val) * lax.rsqrt(var_val + 1e-06) * ln_gain[layer][None, :] + ln_bias[layer][None, :]).astype(jnp.bfloat16)
        branch = jnp.zeros((TOKENS, D), jnp.float32)
        for part_index in range(N_TP):
            piece = jnp.dot(normed[:, part_index * block:(part_index + 1) * block], w_out[layer, part_index * block:(part_index + 1) * block], preferred_element_type=jnp.float32).astype(jnp.bfloat16)
            branch = branch + piece.astype(jnp.float32)
        stream = (xf + branch).astype(jnp.bfloat16)
    return stream
```

```python
import functools

import jax
import jax.numpy as jnp
from jax import lax
from jax.experimental import pallas as pl
from jax.experimental.pallas import tpu as pltpu
from jax.sharding import PartitionSpec as P

MESH = pl.DeviceIdType.MESH
PAIR = 2
CHUNK = 128
HALO = 32
LANES = 128


def fused_kernel(
    n_sp, n_tp, eps,
    x_ref, gain_ref, wv_ref, wg_ref, taps_ref, lng_ref, lnb_ref, wo_ref,
    out_ref,
    wv_all, wg_all, wo_all, xf, hid, glu, filt, rim_out, rim_in, stat,
    ps_out, ps_in, keep, fs_out, fs_in,
    w_recv, w_zsend, w_xsend, ag_recv, ag_send, rim_s, rim_r, st_recv, st_send,
    ps_s, ps_r, fs_s, fs_r,
):
    sp = lax.axis_index("sp")
    tp = lax.axis_index("tp")
    layers, depth = wv_ref.shape[0], wv_ref.shape[1]
    rows, dblk = x_ref.shape
    width = wo_ref.shape[2]
    chan = wv_ref.shape[2]
    taps = taps_ref.shape[1]
    features = dblk * n_tp
    channels = chan * n_tp
    n_chunks = rows // CHUNK
    n_out = n_sp // PAIR
    per_blk = dblk // width
    outer, inner = lax.div(sp, PAIR), lax.rem(sp, PAIR)
    x_peer = outer * PAIR + (PAIR - 1 - inner)
    far_half, core = lax.div(tp, PAIR), lax.rem(tp, PAIR)
    partner = far_half * PAIR + (PAIR - 1 - core)
    far = (n_tp // PAIR - 1 - far_half) * PAIR + core
    far_partner = (n_tp // PAIR - 1 - far_half) * PAIR + (PAIR - 1 - core)
    first_off = HALO - (taps - 1)
    halves = chan // LANES

    barrier = pltpu.get_barrier_semaphore()
    for step in range(1, n_sp):
        pl.semaphore_signal(barrier, inc=1, device_id=(lax.rem(sp + step, n_sp), tp), device_id_type=MESH)
    for step in range(1, n_tp):
        pl.semaphore_signal(barrier, inc=1, device_id=(sp, lax.rem(tp + step, n_tp)), device_id_type=MESH)
    pl.semaphore_wait(barrier, n_sp - 1 + n_tp - 1)

    def chunk_rows(c):
        return pl.ds(pl.multiple_of(c * CHUNK, CHUNK), CHUNK)

    def remote(src, dst, send, recv, sp_to, tp_to):
        return pltpu.make_async_remote_copy(
            src_ref=src, dst_ref=dst, send_sem=send, recv_sem=recv,
            device_id=(sp_to, tp_to), device_id_type=MESH,
        )

    w_in = (wv_ref, wg_ref, wo_ref)

    def w_slot(m, l, s):
        if m == 2:
            return wo_all.at[l, s]
        return (wv_all, wg_all)[m].at[l, pl.ds(pl.multiple_of(s * depth, depth), depth), :]

    def z_copy(m, l, j):
        to = lax.rem(outer + j, n_out) * PAIR + inner
        return remote(w_in[m].at[l], w_slot(m, l, sp), w_zsend.at[l, m, j], w_recv.at[l, m, sp], to, tp)

    def z_arrival(m, l, j):
        s = lax.rem(outer + j, n_out) * PAIR + inner
        return remote(w_in[m].at[l], w_slot(m, l, s), w_zsend.at[l, m, j], w_recv.at[l, m, s], s, tp)

    def x_copy(m, l, j):
        s = lax.rem(outer + j, n_out) * PAIR + inner
        src = w_in[m].at[l] if j == 0 else w_slot(m, l, s)
        return remote(src, w_slot(m, l, s), w_xsend.at[l, m, j], w_recv.at[l, m, s], x_peer, tp)

    def x_arrival(m, l, j):
        s = lax.rem(outer + j, n_out) * PAIR + (PAIR - 1 - inner)
        return remote(w_in[m].at[l], w_slot(m, l, s), w_xsend.at[l, m, j], w_recv.at[l, m, s], x_peer, tp)

    def z_send_all(m, l):
        for j in range(1, n_out):
            z_copy(m, l, j).start()

    def relay(m, l):
        for j in range(1, n_out):
            z_arrival(m, l, j).wait_recv()
            x_copy(m, l, j).start()

    def w_ready(m, l):
        for j in range(n_out):
            x_arrival(m, l, j).wait_recv()

    def ag_far(c):
        r = chunk_rows(c)
        return remote(xf.at[tp, r, :], xf.at[tp, r, :], ag_send.at[0, c], ag_recv.at[0, c], sp, far)

    def ag_partner(c):
        r = chunk_rows(c)
        return remote(xf.at[tp, r, :], xf.at[tp, r, :], ag_send.at[1, c], ag_recv.at[1, c], sp, partner)

    def ag_forward(c):
        r = chunk_rows(c)
        return remote(xf.at[far, r, :], xf.at[far, r, :], ag_send.at[2, c], ag_recv.at[2, c], sp, partner)

    def stat_copy(l, c, step):
        to = lax.rem(tp + step, n_tp)
        return remote(stat.at[l, c, tp], stat.at[l, c, tp], st_send.at[c, step], st_recv.at[c, tp], sp, to)

    def stat_arrival(l, c, step):
        src = lax.rem(tp + step, n_tp)
        return remote(stat.at[l, c, src], stat.at[l, c, src], st_send.at[c, step], st_recv.at[c, src], sp, src)

    def ps_copy(c):
        r = chunk_rows(c)
        return remote(ps_out.at[:, r, :], ps_in.at[:, r, :], ps_s.at[c], ps_r.at[c], sp, partner)

    def fs_copy(c):
        r = chunk_rows(c)
        return remote(fs_out.at[r, :], fs_in.at[r, :], fs_s.at[c], fs_r.at[c], sp, far)

    def rim_copy(l):
        to = lax.rem(sp + 1, n_sp)
        return remote(rim_out.at[l], rim_in.at[l], rim_s.at[l], rim_r.at[l], to, tp)

    xf[tp] = x_ref[...]
    for c in range(n_chunks):
        ag_far(c).start()
        ag_partner(c).start()
    for m in range(3):
        z_send_all(m, 0)
        x_copy(m, 0, 0).start()

    def own_weights(l, carry):
        own = pl.ds(pl.multiple_of(sp * depth, depth), depth)
        wv_all[l, own, :] = wv_ref[l]
        wg_all[l, own, :] = wg_ref[l]
        wo_all[l, sp] = wo_ref[l]
        return carry

    lax.fori_loop(0, layers, own_weights, 0)

    relay(0, 0)
    relay(1, 0)

    def do_glu(l, c):
        ag_partner(c).wait_recv()
        ag_forward(c).wait_recv()
        r = chunk_rows(c)
        blocks = [xf[b, r, :].astype(jnp.float32) for b in range(n_tp)]
        total = sum(jnp.sum(b * b, axis=1, keepdims=True) for b in blocks)
        scale = lax.rsqrt(total / features + eps)
        for b in range(n_tp):
            cols = slice(b * dblk, (b + 1) * dblk)
            hid[:, cols] = (xf[b, r, :].astype(jnp.float32) * scale * gain_ref[l, :, cols]).astype(jnp.bfloat16)
        h = hid[...]
        value = jnp.dot(h, wv_all[l], preferred_element_type=jnp.float32)
        gate = jnp.dot(h, wg_all[l], preferred_element_type=jnp.float32)
        g = (value * jax.nn.sigmoid(gate)).astype(jnp.bfloat16)
        for k in range(halves):
            glu[k, pl.ds(pl.multiple_of(HALO + c * CHUNK, HALO), CHUNK), :] = g[:, k * LANES:(k + 1) * LANES].astype(jnp.float32)

        @pl.when((c == n_chunks - 1) & (sp < n_sp - 1))
        def _():
            rim_out[l] = g[CHUNK - HALO:, :]
            rim_copy(l).start()

    def do_conv(l, c):
        @pl.when((c == 0) & (sp > 0))
        def _():
            rim_copy(l).wait_recv()
            rim = rim_in[l].astype(jnp.float32)
            for k in range(halves):
                glu[k, 0:HALO, :] = rim[:, k * LANES:(k + 1) * LANES]

        @pl.when((c == 0) & (sp == 0))
        def _():
            glu[:, 0:HALO, :] = jnp.zeros((halves, HALO, LANES), jnp.float32)

        r = chunk_rows(c)
        sums = jnp.zeros((CHUNK, 1), jnp.float32)
        squares = jnp.zeros((CHUNK, 1), jnp.float32)
        for k in range(halves):
            acc = jnp.zeros((CHUNK, LANES), jnp.float32)
            for tap in range(taps):
                acc = acc + taps_ref[l, tap:tap + 1, k * LANES:(k + 1) * LANES] * glu[
                    k, pl.ds(c * CHUNK + first_off + tap, CHUNK), :]
            filt[r, k * LANES:(k + 1) * LANES] = acc
            sums = sums + jnp.sum(acc, axis=1, keepdims=True)
            squares = squares + jnp.sum(acc * acc, axis=1, keepdims=True)
        lane = lax.broadcasted_iota(jnp.int32, (CHUNK, LANES), 1)
        both = jnp.where(lane == 0, sums, squares)
        stat[l, c, tp] = jnp.transpose(both)[0:8, :]
        for step in range(1, n_tp):
            stat_copy(l, c, step).start()

    def do_out(l, c):
        for step in range(1, n_tp):
            stat_arrival(l, c, step).wait_recv()
        r = chunk_rows(c)
        tot = stat[l, c, 0]
        for b in range(1, n_tp):
            tot = tot + stat[l, c, b]
        tot = jnp.transpose(jnp.concatenate([tot, jnp.zeros((LANES - 8, CHUNK), jnp.float32)], axis=0))
        mean = tot[:, 0:1] / channels
        var = tot[:, 1:2] / channels - mean * mean
        pre = (filt[r, :] - mean) * lax.rsqrt(var + eps) * lng_ref[l] + lnb_ref[l]
        normed = jax.nn.silu(pre).astype(jnp.bfloat16)
        for step in range(1, n_tp):
            stat_copy(l, c, step).wait_send()
        ag_far(c).wait_send()
        ag_partner(c).wait_send()
        ag_forward(c).wait_send()
        for half in range(n_tp // PAIR):
            for q in range(per_blk):
                cols = slice(q * width, (q + 1) * width)
                away = (half * PAIR + (PAIR - 1 - core)) * per_blk + q
                ps_out[half, r, cols] = jnp.dot(
                    normed, wo_all[l, away], preferred_element_type=jnp.float32).astype(jnp.bfloat16)
        ps_copy(c).start()
        for half in range(n_tp // PAIR):
            for q in range(per_blk):
                cols = slice(q * width, (q + 1) * width)
                mine = (half * PAIR + core) * per_blk + q
                keep[half, r, cols] = jnp.dot(normed, wo_all[l, mine], preferred_element_type=jnp.float32)

    def do_pair(l, c):
        ps_copy(c).wait_recv()
        r = chunk_rows(c)
        other = n_tp // PAIR - 1 - far_half
        fs_out[r, :] = (keep[other, r, :] + ps_in[other, r, :].astype(jnp.float32)).astype(jnp.bfloat16)
        fs_copy(c).start()

    def do_final(l, c):
        fs_copy(c).wait_recv()
        ps_copy(c).wait_send()
        fs_copy(c).wait_send()
        r = chunk_rows(c)
        branch = keep[far_half, r, :] + ps_in[far_half, r, :].astype(jnp.float32) + fs_in[r, :].astype(jnp.float32)
        new = (xf[tp, r, :].astype(jnp.float32) + branch).astype(jnp.bfloat16)

        @pl.when(l < layers - 1)
        def _():
            xf[tp, r, :] = new
            ag_far(c).start()
            ag_partner(c).start()

        @pl.when(l == layers - 1)
        def _():
            out_ref[r, :] = new

    def layer_body(l, carry):
        base = lax.rem(l, n_chunks)
        more = l < layers - 1

        @pl.when(more)
        def _():
            for m in range(3):
                z_send_all(m, l + 1)

        w_ready(0, l)
        w_ready(1, l)

        def step_body(i, inner_carry):
            def at(back):
                return lax.rem(base + i + n_chunks * 2 - back, n_chunks)

            @pl.when(i < n_chunks)
            def _():
                ag_far(at(0)).wait_recv()
                ag_forward(at(0)).start()

            @pl.when((i >= 2) & (i < n_chunks + 2))
            def _():
                do_conv(l, at(1))

            @pl.when(i < n_chunks)
            def _():
                do_glu(l, at(0))

            @pl.when(i == 2)
            def _():
                relay(2, l)

            @pl.when(i == 3)
            def _():
                w_ready(2, l)

            @pl.when((i >= 3) & (i < n_chunks + 3))
            def _():
                do_out(l, at(2))

            @pl.when((i >= 4) & (i < n_chunks + 4))
            def _():
                do_pair(l, at(3))

            @pl.when(more & (i == n_chunks))
            def _():
                for m in range(3):
                    x_copy(m, l + 1, 0).start()

            @pl.when(more & (i == n_chunks + 2))
            def _():
                relay(0, l + 1)

            @pl.when(i >= 5)
            def _():
                do_final(l, at(4))

            return inner_carry

        lax.fori_loop(0, n_chunks + 5, step_body, 0)

        @pl.when(more)
        def _():
            relay(1, l + 1)

        return carry

    lax.fori_loop(0, layers, layer_body, 0)

    def drain(l, carry):
        for m in range(3):
            for j in range(1, n_out):
                z_copy(m, l, j).wait_send()
            for j in range(n_out):
                x_copy(m, l, j).wait_send()

        @pl.when(sp < n_sp - 1)
        def _():
            rim_copy(l).wait_send()

        return carry

    lax.fori_loop(0, layers, drain, 0)


def fused_shards(n_sp, n_tp, inputs, norm_gain, w_value, w_gate, conv_taps, ln_gain, ln_bias, w_out):
    layers, depth, chan = w_value.shape
    rows, dblk = inputs.shape
    width = w_out.shape[2]
    n_chunks = rows // CHUNK
    features = dblk * n_tp
    n_half = n_tp // PAIR
    bf16, f32 = jnp.bfloat16, jnp.float32
    dma = pltpu.SemaphoreType.DMA
    vmem = pl.BlockSpec(memory_space=pltpu.VMEM)
    return pl.pallas_call(
        functools.partial(fused_kernel, n_sp, n_tp, 1e-06),
        out_shape=jax.ShapeDtypeStruct((rows, dblk), bf16),
        in_specs=[vmem] * 8,
        out_specs=vmem,
        scratch_shapes=[
            pltpu.VMEM((layers, n_sp * depth, chan), bf16),
            pltpu.VMEM((layers, n_sp * depth, chan), bf16),
            pltpu.VMEM((layers, n_sp, chan, width), bf16),
            pltpu.VMEM((n_tp, rows, dblk), bf16),
            pltpu.VMEM((CHUNK, features), bf16),
            pltpu.VMEM((chan // LANES, HALO + rows, LANES), f32),
            pltpu.VMEM((rows, chan), f32),
            pltpu.VMEM((layers, HALO, chan), bf16),
            pltpu.VMEM((layers, HALO, chan), bf16),
            pltpu.VMEM((layers, n_chunks, n_tp, 8, CHUNK), f32),
            pltpu.VMEM((n_half, rows, dblk), bf16),
            pltpu.VMEM((n_half, rows, dblk), bf16),
            pltpu.VMEM((n_half, rows, dblk), f32),
            pltpu.VMEM((rows, dblk), bf16),
            pltpu.VMEM((rows, dblk), bf16),
            dma((layers, 3, n_sp)),
            dma((layers, 3, n_sp // PAIR)),
            dma((layers, 3, n_sp // PAIR)),
            dma((3, n_chunks)),
            dma((3, n_chunks)),
            dma((layers,)),
            dma((layers,)),
            dma((n_chunks, n_tp)),
            dma((n_chunks, n_tp)),
            dma((n_chunks,)),
            dma((n_chunks,)),
            dma((n_chunks,)),
            dma((n_chunks,)),
        ],
        compiler_params=pltpu.CompilerParams(collective_id=0, has_side_effects=True),
    )(
        inputs,
        norm_gain.reshape(layers, 1, features),
        w_value,
        w_gate,
        conv_taps,
        ln_gain.reshape(layers, 1, chan),
        ln_bias.reshape(layers, 1, chan),
        w_out,
    )


def fits_kernel(n_sp, n_tp, inputs, w_value, conv_taps, w_out):
    rows, dblk = inputs.shape
    width = w_out.shape[2]
    return (
        n_sp % PAIR == 0
        and n_sp > PAIR
        and n_tp == PAIR * PAIR
        and rows % CHUNK == 0
        and rows // CHUNK >= 2
        and w_value.shape[1] % LANES == 0
        and w_value.shape[2] % LANES == 0
        and width % LANES == 0
        and dblk % width == 0
        and conv_taps.shape[1] - 1 <= HALO
    )


def shards(inputs, norm_gain, w_value, w_gate, conv_taps, ln_gain, ln_bias, w_out):
    n_sp, n_tp = lax.axis_size("sp"), lax.axis_size("tp")
    args = (inputs, norm_gain, w_value, w_gate, conv_taps, ln_gain, ln_bias, w_out)
    if fits_kernel(n_sp, n_tp, inputs, w_value, conv_taps, w_out):
        return fused_shards(n_sp, n_tp, *args)
    return plain_shards(*args)


def from_behind(block, axis, distance):
    devices = range(lax.axis_size(axis))
    route = [(i - distance, i) for i in devices if i - distance in devices]
    return lax.ppermute(block, axis, route)


def plain_shards(inputs, norm_gain, w_value, w_gate, conv_taps, ln_gain, ln_bias, w_out):
    rows = inputs.shape[0]
    reach = conv_taps.shape[1] - 1
    layers = conv_taps.shape[0]
    channels = conv_taps.shape[2] * lax.axis_size("tp")
    whole_value, whole_gate, whole_out = (
        lax.all_gather(w_value, "sp", axis=1, tiled=True),
        lax.all_gather(w_gate, "sp", axis=1, tiled=True),
        lax.all_gather(w_out, "sp", axis=2, tiled=True),
    )
    stream = inputs
    for layer in range(layers):
        full_rows = lax.all_gather(stream, "tp", axis=1, tiled=True)
        xf = full_rows.astype(jnp.float32)
        meansq = jnp.mean(xf * xf, axis=1, keepdims=True)
        hidden = (xf * lax.rsqrt(meansq + 1e-06) * norm_gain[layer][None, :]).astype(jnp.bfloat16)
        value = jnp.dot(hidden, whole_value[layer], preferred_element_type=jnp.float32)
        gate = jnp.dot(hidden, whole_gate[layer], preferred_element_type=jnp.float32)
        glu = (value * jax.nn.sigmoid(gate)).astype(jnp.bfloat16)
        rim = from_behind(glu[rows - reach :], "sp", 1)
        padded = jnp.concatenate([rim, glu], axis=0)
        count = padded.shape[0] - reach
        filtered = jnp.zeros((count, glu.shape[1]), jnp.float32)
        for tap in range(reach + 1):
            filtered = filtered + conv_taps[layer, tap][None, :] * padded[tap : tap + count].astype(
                jnp.float32
            )
        total_sum, total_sq = lax.psum(
            (jnp.sum(filtered, axis=1), jnp.sum(filtered * filtered, axis=1)), "tp"
        )
        mean_val = (total_sum / channels)[:, None]
        var_val = (total_sq / channels)[:, None] - mean_val * mean_val
        normed = jax.nn.silu(
            (filtered - mean_val) * lax.rsqrt(var_val + 1e-06) * ln_gain[layer][None, :]
            + ln_bias[layer][None, :]
        ).astype(jnp.bfloat16)
        partial_out = jnp.dot(normed, whole_out[layer], preferred_element_type=jnp.float32)
        summed = lax.psum_scatter(
            partial_out.astype(jnp.bfloat16), "tp", scatter_dimension=1, tiled=True
        ).astype(jnp.float32)
        kept = stream.astype(jnp.float32)
        stream = (kept + summed).astype(jnp.bfloat16)
    return stream


def solution(mesh):
    in_specs = (
        P("sp", "tp"),
        P(),
        P(None, "sp", "tp"),
        P(None, "sp", "tp"),
        P(None, None, "tp"),
        P(None, "tp"),
        P(None, "tp"),
        P(None, "tp", "sp"),
    )
    out_specs = P("sp", "tp")
    return jax.shard_map(shards, mesh=mesh, in_specs=in_specs, out_specs=out_specs, check_vma=False)
```

```python
import functools

import jax
import jax.numpy as jnp
from jax import lax
from jax.experimental import pallas as pl
from jax.experimental.pallas import tpu as pltpu
from jax.sharding import PartitionSpec as P

MESH = pl.DeviceIdType.MESH
PAIR = 2
CHUNK = 128
HALO = 32
LANES = 128
SIDE = (1,)


def fused_kernel(
    n_sp, n_tp, eps,
    x_ref, gain_ref, wv_ref, wg_ref, taps_ref, lng_ref, lnb_ref, wo_ref,
    out_ref,
    wv_all, wg_all, wo_all, xf, hid, glu, filt, rim_out, rim_in, stat,
    ps_out, ps_in, keep, fs_out, fs_in,
    w_recv, w_zsend, w_xsend, ag_recv, ag_send, rim_s, rim_r, st_recv, st_send,
    ps_s, ps_r, fs_s, fs_r,
):
    sp = lax.axis_index("sp")
    tp = lax.axis_index("tp")
    layers, depth = wv_ref.shape[0], wv_ref.shape[1]
    rows, dblk = x_ref.shape
    width = wo_ref.shape[2]
    chan = wv_ref.shape[2]
    taps = taps_ref.shape[1]
    features = dblk * n_tp
    channels = chan * n_tp
    n_chunks = rows // CHUNK
    n_out = n_sp // PAIR
    per_blk = dblk // width
    outer, inner = lax.div(sp, PAIR), lax.rem(sp, PAIR)
    x_peer = outer * PAIR + (PAIR - 1 - inner)
    far_half, core = lax.div(tp, PAIR), lax.rem(tp, PAIR)
    partner = far_half * PAIR + (PAIR - 1 - core)
    far = (n_tp // PAIR - 1 - far_half) * PAIR + core
    far_partner = (n_tp // PAIR - 1 - far_half) * PAIR + (PAIR - 1 - core)
    first_off = HALO - (taps - 1)
    halves = chan // LANES

    barrier = pltpu.get_barrier_semaphore()
    for step in range(1, n_sp):
        pl.semaphore_signal(barrier, inc=1, device_id=(lax.rem(sp + step, n_sp), tp), device_id_type=MESH)
    for step in range(1, n_tp):
        pl.semaphore_signal(barrier, inc=1, device_id=(sp, lax.rem(tp + step, n_tp)), device_id_type=MESH)
    pl.semaphore_wait(barrier, n_sp - 1 + n_tp - 1)

    def chunk_rows(c):
        return pl.ds(pl.multiple_of(c * CHUNK, CHUNK), CHUNK)

    def remote(src, dst, send, recv, sp_to, tp_to):
        return pltpu.make_async_remote_copy(
            src_ref=src, dst_ref=dst, send_sem=send, recv_sem=recv,
            device_id=(sp_to, tp_to), device_id_type=MESH,
        )

    w_in = (wv_ref, wg_ref, wo_ref)

    def w_slot(m, l, s):
        if m == 2:
            return wo_all.at[l, s]
        return (wv_all, wg_all)[m].at[l, pl.ds(pl.multiple_of(s * depth, depth), depth), :]

    last = n_out - 1
    upper = lax.div(outer, n_out // 2)
    near_end = outer + upper * (last - 2 * outer)

    def line(j):
        near = j + 1 - (near_end if j == 0 else 0)
        return near + upper * (last - 2 * near)

    def z_copy(m, l, j):
        to = line(j) * PAIR + inner
        return remote(w_in[m].at[l], w_slot(m, l, sp), w_zsend.at[l, m, j], w_recv.at[l, m, sp], to, tp)

    def z_arrival(m, l, j):
        s = line(j) * PAIR + inner
        return remote(w_in[m].at[l], w_slot(m, l, s), w_zsend.at[l, m, j], w_recv.at[l, m, s], s, tp)

    def z_forward(m, l):
        s = line(last - 1) * PAIR + inner
        to = upper * last * PAIR + inner
        slot = w_slot(m, l, s)
        return remote(slot, slot, w_zsend.at[l, m, last], w_recv.at[l, m, s], to, tp)

    def x_own(m, l):
        return remote(w_in[m].at[l], w_slot(m, l, sp), w_xsend.at[l, m, last], w_recv.at[l, m, sp], x_peer, tp)

    def x_copy(m, l, j):
        s = line(j) * PAIR + inner
        slot = w_slot(m, l, s)
        return remote(slot, slot, w_xsend.at[l, m, j], w_recv.at[l, m, s], x_peer, tp)

    def x_arrival(m, l, z):
        s = z * PAIR + (PAIR - 1 - inner)
        slot = w_slot(m, l, s)
        return remote(slot, slot, w_xsend.at[l, m, last], w_recv.at[l, m, s], x_peer, tp)

    def side_copy(m, l):
        to = line(0) * PAIR + inner
        slot = w_slot(m, l, x_peer)
        return remote(slot, slot, w_xsend.at[l, m, 0], w_recv.at[l, m, x_peer], to, tp)

    def z_send_all(m, l):
        for j in range(last - 1):
            z_copy(m, l, j).start()

        @pl.when(near_end == 1)
        def _():
            z_copy(m, l, last - 1).start()

    def relay_piece(m, l, j):
        z_arrival(m, l, j).wait_recv()
        if j == 0 and m in SIDE:
            x_arrival(m, l, outer).wait_recv()
            side_copy(m, l).start()
        else:
            x_copy(m, l, j).start()
        if j == last - 1:
            @pl.when(near_end == 1)
            def _():
                z_forward(m, l).start()

    def relay(m, l):
        for j in range(last):
            relay_piece(m, l, j)

    def w_ready(m, l):
        if m not in SIDE:
            x_arrival(m, l, outer).wait_recv()
        for j in range(last):
            x_arrival(m, l, line(j)).wait_recv()

    def ag_far(c):
        r = chunk_rows(c)
        return remote(xf.at[tp, r, :], xf.at[tp, r, :], ag_send.at[0, c], ag_recv.at[0, c], sp, far)

    def ag_partner(c):
        r = chunk_rows(c)
        return remote(xf.at[tp, r, :], xf.at[tp, r, :], ag_send.at[1, c], ag_recv.at[1, c], sp, partner)

    def ag_forward(c):
        r = chunk_rows(c)
        return remote(xf.at[far, r, :], xf.at[far, r, :], ag_send.at[2, c], ag_recv.at[2, c], sp, partner)

    def stat_copy(l, c, step):
        to = lax.rem(tp + step, n_tp)
        return remote(stat.at[l, c, tp], stat.at[l, c, tp], st_send.at[c, step], st_recv.at[c, tp], sp, to)

    def stat_arrival(l, c, step):
        src = lax.rem(tp + step, n_tp)
        return remote(stat.at[l, c, src], stat.at[l, c, src], st_send.at[c, step], st_recv.at[c, src], sp, src)

    def ps_copy(c):
        r = chunk_rows(c)
        return remote(ps_out.at[:, r, :], ps_in.at[:, r, :], ps_s.at[c], ps_r.at[c], sp, partner)

    def fs_copy(c):
        r = chunk_rows(c)
        return remote(fs_out.at[r, :], fs_in.at[r, :], fs_s.at[c], fs_r.at[c], sp, far)

    def rim_copy(l):
        to = lax.rem(sp + 1, n_sp)
        return remote(rim_out.at[l], rim_in.at[l], rim_s.at[l], rim_r.at[l], to, tp)

    xf[tp] = x_ref[...]
    for c in range(n_chunks):
        ag_far(c).start()
        ag_partner(c).start()
    for m in range(2):
        z_send_all(m, 0)
    for m in range(3):
        x_own(m, 0).start()

    def own_weights(l, carry):
        own = pl.ds(pl.multiple_of(sp * depth, depth), depth)
        wv_all[l, own, :] = wv_ref[l]
        wg_all[l, own, :] = wg_ref[l]
        wo_all[l, sp] = wo_ref[l]
        return carry

    lax.fori_loop(0, layers, own_weights, 0)

    z_send_all(2, 0)
    relay(0, 0)
    x_own(0, 1).start()
    z_send_all(0, 1)
    relay(1, 0)
    x_own(1, 1).start()

    def do_glu(l, c):
        ag_partner(c).wait_recv()
        ag_forward(c).wait_recv()
        r = chunk_rows(c)
        blocks = [xf[b, r, :].astype(jnp.float32) for b in range(n_tp)]
        total = sum(jnp.sum(b * b, axis=1, keepdims=True) for b in blocks)
        scale = lax.rsqrt(total / features + eps)
        for b in range(n_tp):
            cols = slice(b * dblk, (b + 1) * dblk)
            hid[:, cols] = (xf[b, r, :].astype(jnp.float32) * scale * gain_ref[pl.ds(l, 1), cols]).astype(jnp.bfloat16)
        h = hid[...]
        value = jnp.dot(h, wv_all[l], preferred_element_type=jnp.float32)
        gate = jnp.dot(h, wg_all[l], preferred_element_type=jnp.float32)
        g = (value * jax.nn.sigmoid(gate)).astype(jnp.bfloat16)
        for k in range(halves):
            glu[k, pl.ds(pl.multiple_of(HALO + c * CHUNK, HALO), CHUNK), :] = g[:, k * LANES:(k + 1) * LANES].astype(jnp.float32)

        @pl.when((c == n_chunks - 1) & (sp < n_sp - 1))
        def _():
            rim_out[l] = g[CHUNK - HALO:, :]
            rim_copy(l).start()

    def do_conv(l, c):
        @pl.when((c == 0) & (sp > 0))
        def _():
            rim_copy(l).wait_recv()
            rim = rim_in[l].astype(jnp.float32)
            for k in range(halves):
                glu[k, 0:HALO, :] = rim[:, k * LANES:(k + 1) * LANES]

        @pl.when((c == 0) & (sp == 0))
        def _():
            glu[:, 0:HALO, :] = jnp.zeros((halves, HALO, LANES), jnp.float32)

        r = chunk_rows(c)
        sums = jnp.zeros((CHUNK, 1), jnp.float32)
        squares = jnp.zeros((CHUNK, 1), jnp.float32)
        for k in range(halves):
            acc = jnp.zeros((CHUNK, LANES), jnp.float32)
            for tap in range(taps):
                acc = acc + taps_ref[l, tap:tap + 1, k * LANES:(k + 1) * LANES] * glu[
                    k, pl.ds(c * CHUNK + first_off + tap, CHUNK), :]
            filt[r, k * LANES:(k + 1) * LANES] = acc
            sums = sums + jnp.sum(acc, axis=1, keepdims=True)
            squares = squares + jnp.sum(acc * acc, axis=1, keepdims=True)
        lane = lax.broadcasted_iota(jnp.int32, (CHUNK, LANES), 1)
        both = jnp.where(lane == 0, sums, squares)
        stat[l, c, tp] = jnp.transpose(both)[0:8, :]
        for step in range(1, n_tp):
            stat_copy(l, c, step).start()

    def do_out(l, c):
        for step in range(1, n_tp):
            stat_arrival(l, c, step).wait_recv()
        r = chunk_rows(c)
        tot = stat[l, c, 0]
        for b in range(1, n_tp):
            tot = tot + stat[l, c, b]
        tot = jnp.transpose(jnp.concatenate([tot, jnp.zeros((LANES - 8, CHUNK), jnp.float32)], axis=0))
        mean = tot[:, 0:1] / channels
        var = tot[:, 1:2] / channels - mean * mean
        pre = (filt[r, :] - mean) * lax.rsqrt(var + eps) * lng_ref[pl.ds(l, 1), :] + lnb_ref[pl.ds(l, 1), :]
        normed = jax.nn.silu(pre).astype(jnp.bfloat16)
        for step in range(1, n_tp):
            stat_copy(l, c, step).wait_send()
        ag_far(c).wait_send()
        ag_partner(c).wait_send()
        ag_forward(c).wait_send()
        for half in range(n_tp // PAIR):
            for q in range(per_blk):
                cols = slice(q * width, (q + 1) * width)
                away = (half * PAIR + (PAIR - 1 - core)) * per_blk + q
                ps_out[half, r, cols] = jnp.dot(
                    normed, wo_all[l, away], preferred_element_type=jnp.float32).astype(jnp.bfloat16)
        ps_copy(c).start()
        for half in range(n_tp // PAIR):
            for q in range(per_blk):
                cols = slice(q * width, (q + 1) * width)
                mine = (half * PAIR + core) * per_blk + q
                keep[half, r, cols] = jnp.dot(normed, wo_all[l, mine], preferred_element_type=jnp.float32)

    def do_pair(l, c):
        ps_copy(c).wait_recv()
        r = chunk_rows(c)
        other = n_tp // PAIR - 1 - far_half
        fs_out[r, :] = (keep[other, r, :] + ps_in[other, r, :].astype(jnp.float32)).astype(jnp.bfloat16)
        fs_copy(c).start()

    def do_final(l, c):
        fs_copy(c).wait_recv()
        ps_copy(c).wait_send()
        fs_copy(c).wait_send()
        r = chunk_rows(c)
        branch = keep[far_half, r, :] + ps_in[far_half, r, :].astype(jnp.float32) + fs_in[r, :].astype(jnp.float32)
        new = (xf[tp, r, :].astype(jnp.float32) + branch).astype(jnp.bfloat16)

        @pl.when(l < layers - 1)
        def _():
            xf[tp, r, :] = new
            ag_far(c).start()
            ag_partner(c).start()

        @pl.when(l == layers - 1)
        def _():
            out_ref[r, :] = new

    def layer_body(l, carry):
        base = lax.rem(l, n_chunks)
        more = l < layers - 1

        w_ready(0, l)
        w_ready(1, l)

        def step_body(i, inner_carry):
            def at(back):
                return lax.rem(base + i + n_chunks * 2 - back, n_chunks)

            for k, (m, ahead) in enumerate(((2, 0), (0, 1), (1, 1))):
                z_next, z_ahead = (m + 2) % 3, ahead + (m + 2) // 3

                @pl.when((i == k * last) & (l + z_ahead < layers))
                def _():
                    z_send_all(z_next, l + z_ahead)

                @pl.when((i == k * last) & (l + ahead + 1 < layers))
                def _():
                    x_own(m, l + ahead + 1).start()

                for j in range(last):
                    @pl.when((i == k * last + j) & (l + ahead < layers))
                    def _():
                        relay_piece(m, l + ahead, j)

            @pl.when(i < n_chunks)
            def _():
                ag_far(at(0)).wait_recv()
                ag_forward(at(0)).start()

            @pl.when((i >= 2) & (i < n_chunks + 2))
            def _():
                do_conv(l, at(1))

            @pl.when(i < n_chunks)
            def _():
                do_glu(l, at(0))

            @pl.when(i == 3)
            def _():
                w_ready(2, l)

            @pl.when((i >= 3) & (i < n_chunks + 3))
            def _():
                do_out(l, at(2))

            @pl.when((i >= 4) & (i < n_chunks + 4))
            def _():
                do_pair(l, at(3))

            @pl.when(i >= 5)
            def _():
                do_final(l, at(4))

            return inner_carry

        lax.fori_loop(0, n_chunks + 5, step_body, 0)

        return carry

    lax.fori_loop(0, layers, layer_body, 0)

    def drain(l, carry):
        for m in range(3):
            for j in range(last - 1):
                z_copy(m, l, j).wait_send()

            @pl.when(near_end == 1)
            def _():
                z_copy(m, l, last - 1).wait_send()
                z_forward(m, l).wait_send()

            for j in range(last):
                (side_copy(m, l) if j == 0 and m in SIDE else x_copy(m, l, j)).wait_send()
            x_own(m, l).wait_send()

        @pl.when(sp < n_sp - 1)
        def _():
            rim_copy(l).wait_send()

        return carry

    lax.fori_loop(0, layers, drain, 0)


def fused_shards(n_sp, n_tp, inputs, norm_gain, w_value, w_gate, conv_taps, ln_gain, ln_bias, w_out):
    layers, depth, chan = w_value.shape
    rows, dblk = inputs.shape
    width = w_out.shape[2]
    n_chunks = rows // CHUNK
    features = dblk * n_tp
    n_half = n_tp // PAIR
    bf16, f32 = jnp.bfloat16, jnp.float32
    dma = pltpu.SemaphoreType.DMA
    vmem = pl.BlockSpec(memory_space=pltpu.VMEM)
    return pl.pallas_call(
        functools.partial(fused_kernel, n_sp, n_tp, 1e-06),
        out_shape=jax.ShapeDtypeStruct((rows, dblk), bf16),
        in_specs=[vmem] * 8,
        out_specs=vmem,
        scratch_shapes=[
            pltpu.VMEM((layers, n_sp * depth, chan), bf16),
            pltpu.VMEM((layers, n_sp * depth, chan), bf16),
            pltpu.VMEM((layers, n_sp, chan, width), bf16),
            pltpu.VMEM((n_tp, rows, dblk), bf16),
            pltpu.VMEM((CHUNK, features), bf16),
            pltpu.VMEM((chan // LANES, HALO + rows, LANES), f32),
            pltpu.VMEM((rows, chan), f32),
            pltpu.VMEM((layers, HALO, chan), bf16),
            pltpu.VMEM((layers, HALO, chan), bf16),
            pltpu.VMEM((layers, n_chunks, n_tp, 8, CHUNK), f32),
            pltpu.VMEM((n_half, rows, dblk), bf16),
            pltpu.VMEM((n_half, rows, dblk), bf16),
            pltpu.VMEM((n_half, rows, dblk), f32),
            pltpu.VMEM((rows, dblk), bf16),
            pltpu.VMEM((rows, dblk), bf16),
            dma((layers, 3, n_sp)),
            dma((layers, 3, n_sp // PAIR)),
            dma((layers, 3, n_sp // PAIR)),
            dma((3, n_chunks)),
            dma((3, n_chunks)),
            dma((layers,)),
            dma((layers,)),
            dma((n_chunks, n_tp)),
            dma((n_chunks, n_tp)),
            dma((n_chunks,)),
            dma((n_chunks,)),
            dma((n_chunks,)),
            dma((n_chunks,)),
        ],
        compiler_params=pltpu.CompilerParams(collective_id=0, has_side_effects=True),
    )(
        inputs,
        norm_gain,
        w_value,
        w_gate,
        conv_taps,
        ln_gain,
        ln_bias,
        w_out,
    )


def fits_kernel(n_sp, n_tp, inputs, w_value, conv_taps, w_out):
    rows, dblk = inputs.shape
    width = w_out.shape[2]
    return (
        n_sp == 4 * PAIR
        and n_tp == PAIR * PAIR
        and rows % CHUNK == 0
        and rows // CHUNK >= 4
        and w_value.shape[0] >= 2
        and w_value.shape[1] % LANES == 0
        and w_value.shape[2] % LANES == 0
        and width % LANES == 0
        and dblk % width == 0
        and conv_taps.shape[1] - 1 <= HALO
    )


def shards(inputs, norm_gain, w_value, w_gate, conv_taps, ln_gain, ln_bias, w_out):
    n_sp, n_tp = lax.axis_size("sp"), lax.axis_size("tp")
    args = (inputs, norm_gain, w_value, w_gate, conv_taps, ln_gain, ln_bias, w_out)
    if fits_kernel(n_sp, n_tp, inputs, w_value, conv_taps, w_out):
        return fused_shards(n_sp, n_tp, *args)
    return plain_shards(*args)


def from_behind(block, axis, distance):
    devices = range(lax.axis_size(axis))
    route = [(i - distance, i) for i in devices if i - distance in devices]
    return lax.ppermute(block, axis, route)


def plain_shards(inputs, norm_gain, w_value, w_gate, conv_taps, ln_gain, ln_bias, w_out):
    rows = inputs.shape[0]
    reach = conv_taps.shape[1] - 1
    layers = conv_taps.shape[0]
    channels = conv_taps.shape[2] * lax.axis_size("tp")
    whole_value, whole_gate, whole_out = (
        lax.all_gather(w_value, "sp", axis=1, tiled=True),
        lax.all_gather(w_gate, "sp", axis=1, tiled=True),
        lax.all_gather(w_out, "sp", axis=2, tiled=True),
    )
    stream = inputs
    for layer in range(layers):
        full_rows = lax.all_gather(stream, "tp", axis=1, tiled=True)
        xf = full_rows.astype(jnp.float32)
        meansq = jnp.mean(xf * xf, axis=1, keepdims=True)
        hidden = (xf * lax.rsqrt(meansq + 1e-06) * norm_gain[layer][None, :]).astype(jnp.bfloat16)
        value = jnp.dot(hidden, whole_value[layer], preferred_element_type=jnp.float32)
        gate = jnp.dot(hidden, whole_gate[layer], preferred_element_type=jnp.float32)
        glu = (value * jax.nn.sigmoid(gate)).astype(jnp.bfloat16)
        rim = from_behind(glu[rows - reach :], "sp", 1)
        padded = jnp.concatenate([rim, glu], axis=0)
        count = padded.shape[0] - reach
        filtered = jnp.zeros((count, glu.shape[1]), jnp.float32)
        for tap in range(reach + 1):
            filtered = filtered + conv_taps[layer, tap][None, :] * padded[tap : tap + count].astype(
                jnp.float32
            )
        total_sum, total_sq = lax.psum(
            (jnp.sum(filtered, axis=1), jnp.sum(filtered * filtered, axis=1)), "tp"
        )
        mean_val = (total_sum / channels)[:, None]
        var_val = (total_sq / channels)[:, None] - mean_val * mean_val
        normed = jax.nn.silu(
            (filtered - mean_val) * lax.rsqrt(var_val + 1e-06) * ln_gain[layer][None, :]
            + ln_bias[layer][None, :]
        ).astype(jnp.bfloat16)
        partial_out = jnp.dot(normed, whole_out[layer], preferred_element_type=jnp.float32)
        summed = lax.psum_scatter(
            partial_out.astype(jnp.bfloat16), "tp", scatter_dimension=1, tiled=True
        ).astype(jnp.float32)
        kept = stream.astype(jnp.float32)
        stream = (kept + summed).astype(jnp.bfloat16)
    return stream


def solution(mesh):
    in_specs = (
        P("sp", "tp"),
        P(),
        P(None, "sp", "tp"),
        P(None, "sp", "tp"),
        P(None, None, "tp"),
        P(None, "tp"),
        P(None, "tp"),
        P(None, "tp", "sp"),
    )
    out_specs = P("sp", "tp")
    return jax.shard_map(shards, mesh=mesh, in_specs=in_specs, out_specs=out_specs, check_vma=False)
```

```python
import functools

import jax
import jax.numpy as jnp
from jax import lax
from jax.experimental import pallas as pl
from jax.experimental.pallas import tpu as pltpu
from jax.sharding import PartitionSpec as P

MESH = pl.DeviceIdType.MESH
PAIR = 2
CHUNK = 128
HALO = 32
LANES = 128
FIRST = 6
Z_AHEAD, X_AHEAD = 1, 2
STEPS = (0, 1, 2, 4, 5, 6, 7, 8, 8)
SIDE = (1,)


def fused_kernel(
    n_sp, n_tp, eps,
    x_ref, gain_ref, wv_ref, wg_ref, taps_ref, lng_ref, lnb_ref, wo_ref,
    out_ref,
    wv_all, wg_all, wo_all, xf, hid, glu, filt, rim_out, rim_in, stat,
    ps_out, ps_in, keep, fs_out, fs_in,
    w_recv, w_zsend, w_xsend, ag_recv, ag_send, rim_s, rim_r, st_recv, st_send,
    ps_s, ps_r, fs_s, fs_r,
):
    sp = lax.axis_index("sp")
    tp = lax.axis_index("tp")
    layers, depth = wv_ref.shape[0], wv_ref.shape[1]
    rows, dblk = x_ref.shape
    width = wo_ref.shape[2]
    chan = wv_ref.shape[2]
    taps = taps_ref.shape[1]
    features = dblk * n_tp
    channels = chan * n_tp
    n_chunks = rows // CHUNK
    n_out = n_sp // PAIR
    per_blk = dblk // width
    outer, inner = lax.div(sp, PAIR), lax.rem(sp, PAIR)
    x_peer = outer * PAIR + (PAIR - 1 - inner)
    far_half, core = lax.div(tp, PAIR), lax.rem(tp, PAIR)
    partner = far_half * PAIR + (PAIR - 1 - core)
    far = (n_tp // PAIR - 1 - far_half) * PAIR + core
    far_partner = (n_tp // PAIR - 1 - far_half) * PAIR + (PAIR - 1 - core)
    first_off = HALO - (taps - 1)
    halves = chan // LANES

    barrier = pltpu.get_barrier_semaphore()
    for step in range(1, n_sp):
        pl.semaphore_signal(barrier, inc=1, device_id=(lax.rem(sp + step, n_sp), tp), device_id_type=MESH)
    for step in range(1, n_tp):
        pl.semaphore_signal(barrier, inc=1, device_id=(sp, lax.rem(tp + step, n_tp)), device_id_type=MESH)
    xf[tp] = x_ref[...]

    def own_weights(l, carry):
        own = pl.ds(pl.multiple_of(sp * depth, depth), depth)
        wv_all[l, own, :] = wv_ref[l]
        wg_all[l, own, :] = wg_ref[l]
        wo_all[l, sp] = wo_ref[l]
        return carry

    lax.fori_loop(0, layers, own_weights, 0)
    pl.semaphore_wait(barrier, n_sp - 1 + n_tp - 1)

    def chunk_rows(c):
        return pl.ds(pl.multiple_of(c * CHUNK, CHUNK), CHUNK)

    def remote(src, dst, send, recv, sp_to, tp_to):
        return pltpu.make_async_remote_copy(
            src_ref=src, dst_ref=dst, send_sem=send, recv_sem=recv,
            device_id=(sp_to, tp_to), device_id_type=MESH,
        )

    w_in = (wv_ref, wg_ref, wo_ref)

    def w_slot(m, l, s):
        if m == 2:
            return wo_all.at[l, s]
        return (wv_all, wg_all)[m].at[l, pl.ds(pl.multiple_of(s * depth, depth), depth), :]

    last = n_out - 1
    upper = lax.div(outer, n_out // 2)
    near_end = outer + upper * (last - 2 * outer)

    def line(j):
        near = j + 1 - (near_end if j == 0 else 0)
        return near + upper * (last - 2 * near)

    def z_copy(m, l, j):
        to = line(j) * PAIR + inner
        return remote(w_in[m].at[l], w_slot(m, l, sp), w_zsend.at[l, m, j], w_recv.at[l, m, sp], to, tp)

    def z_arrival(m, l, j):
        s = line(j) * PAIR + inner
        return remote(w_in[m].at[l], w_slot(m, l, s), w_zsend.at[l, m, j], w_recv.at[l, m, s], s, tp)

    def z_forward(m, l):
        s = line(last - 1) * PAIR + inner
        to = upper * last * PAIR + inner
        slot = w_slot(m, l, s)
        return remote(slot, slot, w_zsend.at[l, m, last], w_recv.at[l, m, s], to, tp)

    def x_own(m, l):
        return remote(w_in[m].at[l], w_slot(m, l, sp), w_xsend.at[l, m, last], w_recv.at[l, m, sp], x_peer, tp)

    def x_copy(m, l, j):
        s = line(j) * PAIR + inner
        slot = w_slot(m, l, s)
        return remote(slot, slot, w_xsend.at[l, m, j], w_recv.at[l, m, s], x_peer, tp)

    def x_arrival(m, l, z):
        s = z * PAIR + (PAIR - 1 - inner)
        slot = w_slot(m, l, s)
        return remote(slot, slot, w_xsend.at[l, m, last], w_recv.at[l, m, s], x_peer, tp)

    def side_copy(m, l):
        to = line(0) * PAIR + inner
        slot = w_slot(m, l, x_peer)
        return remote(slot, slot, w_xsend.at[l, m, 0], w_recv.at[l, m, x_peer], to, tp)

    def z_send_all(m, l):
        for j in range(last - 1):
            z_copy(m, l, j).start()

        @pl.when(near_end == 1)
        def _():
            z_copy(m, l, last - 1).start()

    def relay_piece(m, l, j):
        z_arrival(m, l, j).wait_recv()
        if j == 0 and m in SIDE:
            x_arrival(m, l, outer).wait_recv()
            side_copy(m, l).start()
        else:
            x_copy(m, l, j).start()
        if j == last - 1:
            @pl.when(near_end == 1)
            def _():
                z_forward(m, l).start()

    def relay(m, l):
        for j in range(last):
            relay_piece(m, l, j)

    def w_ready(m, l):
        if m not in SIDE:
            x_arrival(m, l, outer).wait_recv()
        for j in range(last):
            x_arrival(m, l, line(j)).wait_recv()

    def ag_far(c):
        r = chunk_rows(c)
        return remote(xf.at[tp, r, :], xf.at[tp, r, :], ag_send.at[0, c], ag_recv.at[0, c], sp, far)

    def ag_partner(c):
        r = chunk_rows(c)
        return remote(xf.at[tp, r, :], xf.at[tp, r, :], ag_send.at[1, c], ag_recv.at[1, c], sp, partner)

    def ag_forward(c):
        r = chunk_rows(c)
        return remote(xf.at[far, r, :], xf.at[far, r, :], ag_send.at[2, c], ag_recv.at[2, c], sp, partner)

    def stat_copy(l, c, step):
        to = lax.rem(tp + step, n_tp)
        return remote(stat.at[l, c, tp], stat.at[l, c, tp], st_send.at[c, step], st_recv.at[c, tp], sp, to)

    def stat_arrival(l, c, step):
        src = lax.rem(tp + step, n_tp)
        return remote(stat.at[l, c, src], stat.at[l, c, src], st_send.at[c, step], st_recv.at[c, src], sp, src)

    def ps_copy(c):
        r = chunk_rows(c)
        return remote(ps_out.at[:, r, :], ps_in.at[:, r, :], ps_s.at[c], ps_r.at[c], sp, partner)

    def fs_copy(c):
        r = chunk_rows(c)
        return remote(fs_out.at[r, :], fs_in.at[r, :], fs_s.at[c], fs_r.at[c], sp, far)

    def rim_copy(l):
        to = lax.rem(sp + 1, n_sp)
        return remote(rim_out.at[l], rim_in.at[l], rim_s.at[l], rim_r.at[l], to, tp)

    for c in range(n_chunks):
        ag_far(c).start()
        ag_partner(c).start()
    for q in range(Z_AHEAD):
        z_send_all(q % 3, q // 3)
    for q in range(X_AHEAD):
        x_own(q % 3, q // 3).start()
    for p in range(FIRST):
        q, j = divmod(p, last)
        if j == 0:
            z_send_all((q + Z_AHEAD) % 3, (q + Z_AHEAD) // 3)
            x_own((q + X_AHEAD) % 3, (q + X_AHEAD) // 3).start()
        relay_piece(q % 3, q // 3, j)

    def do_glu(l, c):
        ag_partner(c).wait_recv()
        ag_forward(c).wait_recv()
        r = chunk_rows(c)
        blocks = [xf[b, r, :].astype(jnp.float32) for b in range(n_tp)]
        total = sum(jnp.sum(b * b, axis=1, keepdims=True) for b in blocks)
        scale = lax.rsqrt(total / features + eps)
        for b in range(n_tp):
            cols = slice(b * dblk, (b + 1) * dblk)
            hid[:, cols] = (xf[b, r, :].astype(jnp.float32) * scale * gain_ref[pl.ds(l, 1), cols]).astype(jnp.bfloat16)
        h = hid[...]
        value = jnp.dot(h, wv_all[l], preferred_element_type=jnp.float32)
        gate = jnp.dot(h, wg_all[l], preferred_element_type=jnp.float32)
        g = (value * jax.nn.sigmoid(gate)).astype(jnp.bfloat16)
        for k in range(halves):
            glu[k, pl.ds(pl.multiple_of(HALO + c * CHUNK, HALO), CHUNK), :] = g[:, k * LANES:(k + 1) * LANES].astype(jnp.float32)

        @pl.when((c == n_chunks - 1) & (sp < n_sp - 1))
        def _():
            rim_out[l] = g[CHUNK - HALO:, :]
            rim_copy(l).start()

    def do_conv(l, c):
        @pl.when((c == 0) & (sp > 0))
        def _():
            rim_copy(l).wait_recv()
            rim = rim_in[l].astype(jnp.float32)
            for k in range(halves):
                glu[k, 0:HALO, :] = rim[:, k * LANES:(k + 1) * LANES]

        @pl.when((c == 0) & (sp == 0))
        def _():
            glu[:, 0:HALO, :] = jnp.zeros((halves, HALO, LANES), jnp.float32)

        r = chunk_rows(c)
        sums = jnp.zeros((CHUNK, 1), jnp.float32)
        squares = jnp.zeros((CHUNK, 1), jnp.float32)
        for k in range(halves):
            acc = jnp.zeros((CHUNK, LANES), jnp.float32)
            for tap in range(taps):
                acc = acc + taps_ref[l, tap:tap + 1, k * LANES:(k + 1) * LANES] * glu[
                    k, pl.ds(c * CHUNK + first_off + tap, CHUNK), :]
            filt[r, k * LANES:(k + 1) * LANES] = acc
            sums = sums + jnp.sum(acc, axis=1, keepdims=True)
            squares = squares + jnp.sum(acc * acc, axis=1, keepdims=True)
        lane = lax.broadcasted_iota(jnp.int32, (CHUNK, LANES), 1)
        both = jnp.where(lane == 0, sums, squares)
        stat[l, c, tp] = jnp.transpose(both)[0:8, :]
        for step in range(1, n_tp):
            stat_copy(l, c, step).start()

    def do_out(l, c):
        for step in range(1, n_tp):
            stat_arrival(l, c, step).wait_recv()
        r = chunk_rows(c)
        tot = stat[l, c, 0]
        for b in range(1, n_tp):
            tot = tot + stat[l, c, b]
        tot = jnp.transpose(jnp.concatenate([tot, jnp.zeros((LANES - 8, CHUNK), jnp.float32)], axis=0))
        mean = tot[:, 0:1] / channels
        var = tot[:, 1:2] / channels - mean * mean
        pre = (filt[r, :] - mean) * lax.rsqrt(var + eps) * lng_ref[pl.ds(l, 1), :] + lnb_ref[pl.ds(l, 1), :]
        normed = jax.nn.silu(pre).astype(jnp.bfloat16)
        for step in range(1, n_tp):
            stat_copy(l, c, step).wait_send()
        ag_far(c).wait_send()
        ag_partner(c).wait_send()
        ag_forward(c).wait_send()
        for half in range(n_tp // PAIR):
            for q in range(per_blk):
                cols = slice(q * width, (q + 1) * width)
                away = (half * PAIR + (PAIR - 1 - core)) * per_blk + q
                ps_out[half, r, cols] = jnp.dot(
                    normed, wo_all[l, away], preferred_element_type=jnp.float32).astype(jnp.bfloat16)
        ps_copy(c).start()
        for half in range(n_tp // PAIR):
            for q in range(per_blk):
                cols = slice(q * width, (q + 1) * width)
                mine = (half * PAIR + core) * per_blk + q
                keep[half, r, cols] = jnp.dot(normed, wo_all[l, mine], preferred_element_type=jnp.float32)

    def do_pair(l, c):
        ps_copy(c).wait_recv()
        r = chunk_rows(c)
        other = n_tp // PAIR - 1 - far_half
        fs_out[r, :] = (keep[other, r, :] + ps_in[other, r, :].astype(jnp.float32)).astype(jnp.bfloat16)
        fs_copy(c).start()

    def do_final(l, c):
        fs_copy(c).wait_recv()
        ps_copy(c).wait_send()
        fs_copy(c).wait_send()
        r = chunk_rows(c)
        branch = keep[far_half, r, :] + ps_in[far_half, r, :].astype(jnp.float32) + fs_in[r, :].astype(jnp.float32)
        new = (xf[tp, r, :].astype(jnp.float32) + branch).astype(jnp.bfloat16)

        @pl.when(l < layers - 1)
        def _():
            xf[tp, r, :] = new
            ag_far(c).start()
            ag_partner(c).start()

        @pl.when(l == layers - 1)
        def _():
            out_ref[r, :] = new

    def layer_body(l, carry):
        base = lax.rem(l, n_chunks)
        more = l < layers - 1

        def step_body(i, inner_carry):
            def at(back):
                return lax.rem(base + i + n_chunks * 2 - back, n_chunks)

            for k in range(3 * last):
                q, j = divmod(FIRST + k, last)
                if j == 0:
                    z_next, x_next = q + Z_AHEAD, q + X_AHEAD

                    @pl.when((i == STEPS[k]) & (l + z_next // 3 < layers))
                    def _():
                        z_send_all(z_next % 3, l + z_next // 3)

                    @pl.when((i == STEPS[k]) & (l + x_next // 3 < layers))
                    def _():
                        x_own(x_next % 3, l + x_next // 3).start()

                @pl.when((i == STEPS[k]) & (l + q // 3 < layers))
                def _():
                    relay_piece(q % 3, l + q // 3, j)

            @pl.when(i < n_chunks)
            def _():
                ag_far(at(0)).wait_recv()
                ag_forward(at(0)).start()

            @pl.when(i == 0)
            def _():
                w_ready(0, l)
                w_ready(1, l)

            @pl.when((i >= 2) & (i < n_chunks + 2))
            def _():
                do_conv(l, at(1))

            @pl.when(i < n_chunks)
            def _():
                do_glu(l, at(0))

            @pl.when(i == 3)
            def _():
                w_ready(2, l)

            @pl.when((i >= 3) & (i < n_chunks + 3))
            def _():
                do_out(l, at(2))

            @pl.when((i >= 4) & (i < n_chunks + 4))
            def _():
                do_pair(l, at(3))

            @pl.when(i >= 5)
            def _():
                do_final(l, at(4))

            return inner_carry

        lax.fori_loop(0, n_chunks + 5, step_body, 0)

        return carry

    lax.fori_loop(0, layers, layer_body, 0)

    def drain(l, carry):
        for m in range(3):
            for j in range(last - 1):
                z_copy(m, l, j).wait_send()

            @pl.when(near_end == 1)
            def _():
                z_copy(m, l, last - 1).wait_send()
                z_forward(m, l).wait_send()

            for j in range(last):
                (side_copy(m, l) if j == 0 and m in SIDE else x_copy(m, l, j)).wait_send()
            x_own(m, l).wait_send()

        @pl.when(sp < n_sp - 1)
        def _():
            rim_copy(l).wait_send()

        return carry

    lax.fori_loop(0, layers, drain, 0)


def fused_shards(n_sp, n_tp, inputs, norm_gain, w_value, w_gate, conv_taps, ln_gain, ln_bias, w_out):
    layers, depth, chan = w_value.shape
    rows, dblk = inputs.shape
    width = w_out.shape[2]
    n_chunks = rows // CHUNK
    features = dblk * n_tp
    n_half = n_tp // PAIR
    bf16, f32 = jnp.bfloat16, jnp.float32
    dma = pltpu.SemaphoreType.DMA
    vmem = pl.BlockSpec(memory_space=pltpu.VMEM)
    return pl.pallas_call(
        functools.partial(fused_kernel, n_sp, n_tp, 1e-06),
        out_shape=jax.ShapeDtypeStruct((rows, dblk), bf16),
        in_specs=[vmem] * 8,
        out_specs=vmem,
        scratch_shapes=[
            pltpu.VMEM((layers, n_sp * depth, chan), bf16),
            pltpu.VMEM((layers, n_sp * depth, chan), bf16),
            pltpu.VMEM((layers, n_sp, chan, width), bf16),
            pltpu.VMEM((n_tp, rows, dblk), bf16),
            pltpu.VMEM((CHUNK, features), bf16),
            pltpu.VMEM((chan // LANES, HALO + rows, LANES), f32),
            pltpu.VMEM((rows, chan), f32),
            pltpu.VMEM((layers, HALO, chan), bf16),
            pltpu.VMEM((layers, HALO, chan), bf16),
            pltpu.VMEM((layers, n_chunks, n_tp, 8, CHUNK), f32),
            pltpu.VMEM((n_half, rows, dblk), bf16),
            pltpu.VMEM((n_half, rows, dblk), bf16),
            pltpu.VMEM((n_half, rows, dblk), f32),
            pltpu.VMEM((rows, dblk), bf16),
            pltpu.VMEM((rows, dblk), bf16),
            dma((layers, 3, n_sp)),
            dma((layers, 3, n_sp // PAIR)),
            dma((layers, 3, n_sp // PAIR)),
            dma((3, n_chunks)),
            dma((3, n_chunks)),
            dma((layers,)),
            dma((layers,)),
            dma((n_chunks, n_tp)),
            dma((n_chunks, n_tp)),
            dma((n_chunks,)),
            dma((n_chunks,)),
            dma((n_chunks,)),
            dma((n_chunks,)),
        ],
        compiler_params=pltpu.CompilerParams(collective_id=0, has_side_effects=True),
    )(
        inputs,
        norm_gain,
        w_value,
        w_gate,
        conv_taps,
        ln_gain,
        ln_bias,
        w_out,
    )


def fits_kernel(n_sp, n_tp, inputs, w_value, conv_taps, w_out):
    rows, dblk = inputs.shape
    width = w_out.shape[2]
    return (
        n_sp == 4 * PAIR
        and n_tp == PAIR * PAIR
        and rows % CHUNK == 0
        and rows // CHUNK >= 4
        and w_value.shape[0] >= 2
        and w_value.shape[1] % LANES == 0
        and w_value.shape[2] % LANES == 0
        and width % LANES == 0
        and dblk % width == 0
        and conv_taps.shape[1] - 1 <= HALO
    )


def shards(inputs, norm_gain, w_value, w_gate, conv_taps, ln_gain, ln_bias, w_out):
    n_sp, n_tp = lax.axis_size("sp"), lax.axis_size("tp")
    args = (inputs, norm_gain, w_value, w_gate, conv_taps, ln_gain, ln_bias, w_out)
    if fits_kernel(n_sp, n_tp, inputs, w_value, conv_taps, w_out):
        return fused_shards(n_sp, n_tp, *args)
    return plain_shards(*args)


def from_behind(block, axis, distance):
    devices = range(lax.axis_size(axis))
    route = [(i - distance, i) for i in devices if i - distance in devices]
    return lax.ppermute(block, axis, route)


def plain_shards(inputs, norm_gain, w_value, w_gate, conv_taps, ln_gain, ln_bias, w_out):
    rows = inputs.shape[0]
    reach = conv_taps.shape[1] - 1
    layers = conv_taps.shape[0]
    channels = conv_taps.shape[2] * lax.axis_size("tp")
    whole_value, whole_gate, whole_out = (
        lax.all_gather(w_value, "sp", axis=1, tiled=True),
        lax.all_gather(w_gate, "sp", axis=1, tiled=True),
        lax.all_gather(w_out, "sp", axis=2, tiled=True),
    )
    stream = inputs
    for layer in range(layers):
        full_rows = lax.all_gather(stream, "tp", axis=1, tiled=True)
        xf = full_rows.astype(jnp.float32)
        meansq = jnp.mean(xf * xf, axis=1, keepdims=True)
        hidden = (xf * lax.rsqrt(meansq + 1e-06) * norm_gain[layer][None, :]).astype(jnp.bfloat16)
        value = jnp.dot(hidden, whole_value[layer], preferred_element_type=jnp.float32)
        gate = jnp.dot(hidden, whole_gate[layer], preferred_element_type=jnp.float32)
        glu = (value * jax.nn.sigmoid(gate)).astype(jnp.bfloat16)
        rim = from_behind(glu[rows - reach :], "sp", 1)
        padded = jnp.concatenate([rim, glu], axis=0)
        count = padded.shape[0] - reach
        filtered = jnp.zeros((count, glu.shape[1]), jnp.float32)
        for tap in range(reach + 1):
            filtered = filtered + conv_taps[layer, tap][None, :] * padded[tap : tap + count].astype(
                jnp.float32
            )
        total_sum, total_sq = lax.psum(
            (jnp.sum(filtered, axis=1), jnp.sum(filtered * filtered, axis=1)), "tp"
        )
        mean_val = (total_sum / channels)[:, None]
        var_val = (total_sq / channels)[:, None] - mean_val * mean_val
        normed = jax.nn.silu(
            (filtered - mean_val) * lax.rsqrt(var_val + 1e-06) * ln_gain[layer][None, :]
            + ln_bias[layer][None, :]
        ).astype(jnp.bfloat16)
        partial_out = jnp.dot(normed, whole_out[layer], preferred_element_type=jnp.float32)
        summed = lax.psum_scatter(
            partial_out.astype(jnp.bfloat16), "tp", scatter_dimension=1, tiled=True
        ).astype(jnp.float32)
        kept = stream.astype(jnp.float32)
        stream = (kept + summed).astype(jnp.bfloat16)
    return stream


def solution(mesh):
    in_specs = (
        P("sp", "tp"),
        P(),
        P(None, "sp", "tp"),
        P(None, "sp", "tp"),
        P(None, None, "tp"),
        P(None, "tp"),
        P(None, "tp"),
        P(None, "tp", "sp"),
    )
    out_specs = P("sp", "tp")
    return jax.shard_map(shards, mesh=mesh, in_specs=in_specs, out_specs=out_specs, check_vma=False)
```
